32 devices in a mesh: ep: 8 (over z, x), tp: 4 (over y, core).
Axes of the slice: x: 2, y: 2, z: 4, core: 2. Of those that a mesh axis runs over, the one named last changes fastest.
Arguments:
- mix_query: bfloat16 [16384, 2048], P('ep', 'tp'), may hold values from -6 to 6
- mix_key: bfloat16 [16384, 2048], P('ep', 'tp'), may hold values from -6 to 6
- mix_value: bfloat16 [16384, 2048], P('ep', 'tp'), may hold values from -6 to 6
- mix_gate: bfloat16 [16384, 2048], P('ep', 'tp'), may hold values from -6 to 6
- log_decay: float32 [16384, 8], P('ep', 'tp'), may hold values from -1 to 0, as said below
- ret_gain: float32 [2048], P('tp'), may hold values from 0.1 to 1.9
- w_out: bfloat16 [2048, 2048], replicated, may hold values from -0.125 to 0.125
- moe_in: bfloat16 [1024, 2048], P(('ep', 'tp')), may hold values from -6 to 6
- route_ids: int32 [1024, 2], P(('ep', 'tp')), may hold values from 0 to 7, as said below
- route_weights: float32 [1024, 2], P(('ep', 'tp')), may hold values from 0.1 to 1
- moe_gain: float32 [2048], replicated, may hold values from 0.1 to 1.9
- w_gate: bfloat16 [8, 2048, 7168], P('ep', None, 'tp'), may hold values from -0.125 to 0.125
- w_up: bfloat16 [8, 2048, 7168], P('ep', None, 'tp'), may hold values from -0.125 to 0.125
- w_down: bfloat16 [8, 7168, 2048], P('ep', 'tp'), may hold values from -0.0625 to 0.0625
Outputs:
- mix_out: bfloat16 [16384, 2048], P(('ep', 'tp'))
- moe_out: bfloat16 [1024, 2048], P(('ep', 'tp'))
The draws below stay inside these ranges and needn't reach their ends.
Inputs may be any that keep to these rules, and one draw needn't show every extreme that they name: `log_decay`: log of a decay. `route_ids`: each row names 2 different experts. Among the rows of one device no expert is named by more than 16 rows, and one expert is named by exactly 16 rows of every device.
All inputs are finite; a program needn't handle non-finite values.
Results may differ from the reference program's by a relative error of at most 0.015.
Values may be sent and summed in bfloat16 or wider, within the bound.
A program may use at most 128 MiB of HBM per device.

```python
import math
import jax
import jax.numpy as jnp
from jax import lax

D = 2048
FF = 7168
RETENTION_HEADS = 8
HEAD_DIM = 256
BLOCK = 512
TOP = 2
SEQ_DEV = 2048
MOE_DEV = 32
SEQUENCE_LENGTH = 16384
MOE_TOK = 1024
EXPERTS = 8
CAP = 16
N_TP = 4


def block_permutation(perm_key, length):
    return jax.random.permutation(perm_key, length)


def draw_route_ids(key, part):
    block_count = MOE_TOK // MOE_DEV
    half_cap = CAP // 2
    pair_count = (EXPERTS - 2) // 2
    base_key = jax.random.fold_in(key, 31)
    key_star, key_order, key_delta, key_shuffle = jax.random.split(base_key, 4)
    star = jax.random.randint(key_star, (), 0, EXPERTS)
    others = (star + 1 + jnp.arange(EXPERTS - 1, dtype=jnp.int32)) % EXPERTS
    order_keys = jax.random.split(key_order, block_count)
    orders = jax.vmap(block_permutation, in_axes=(0, None))(order_keys, EXPERTS - 1)
    ranked = others[orders]
    delta = jax.random.randint(key_delta, (block_count, pair_count), 0, half_cap + 1)
    pair_counts = jnp.stack([half_cap + delta, half_cap - delta], axis=-1).reshape(block_count, 2 * pair_count)
    counts = jnp.concatenate([jnp.full((block_count, 1), CAP, jnp.int32), pair_counts.astype(jnp.int32), jnp.zeros((block_count, 1), jnp.int32)], axis=1)
    listed = jnp.concatenate([jnp.full((block_count, 1), star, jnp.int32), ranked.astype(jnp.int32)], axis=1)
    bounds = jnp.cumsum(counts, axis=1)
    slots = jnp.arange(2 * MOE_DEV, dtype=jnp.int32)
    position = jnp.sum((slots[None, :, None] >= bounds[:, None, :]).astype(jnp.int32), axis=-1)
    chosen = jnp.take_along_axis(listed, position, axis=1)
    paired = jnp.stack([chosen[:, :MOE_DEV], chosen[:, MOE_DEV:]], axis=-1)
    shuffle_keys = jax.random.split(key_shuffle, block_count)
    shuffles = jax.vmap(block_permutation, in_axes=(0, None))(shuffle_keys, MOE_DEV)
    paired = jnp.take_along_axis(paired, shuffles[:, :, None], axis=1)
    return paired.reshape(MOE_TOK, TOP).astype(jnp.int32)


def draw_log_decay(key, part):
    base_key = jax.random.fold_in(key, 53)
    random_keys = jax.random.split(base_key, 6)
    fast_heads = jax.random.uniform(random_keys[0], (RETENTION_HEADS,)) < 0.5
    fast_rate = 1.0 / jax.random.uniform(random_keys[1], (RETENTION_HEADS,), minval=30.0, maxval=100.0)
    slow_rate = jax.random.uniform(random_keys[2], (RETENTION_HEADS,), minval=0.05, maxval=0.2) * math.log(10.0) / SEQUENCE_LENGTH
    per_head_decay = jnp.where(fast_heads, fast_rate, slow_rate)
    device_factor = jnp.exp(jax.random.uniform(random_keys[3], (SEQUENCE_LENGTH // SEQ_DEV,), minval=math.log(0.5), maxval=math.log(2.0)))
    position_index = jnp.arange(SEQUENCE_LENGTH, dtype=jnp.int32)
    decay_factor_lookup = device_factor[position_index // SEQ_DEV]
    spike_position = jax.random.randint(random_keys[4], (RETENTION_HEADS, 2), 0, SEQUENCE_LENGTH)
    spike_length = jnp.log(jax.random.uniform(random_keys[5], (RETENTION_HEADS, 2), minval=0.5, maxval=0.8))
    spike_matches = position_index[:, None, None] == spike_position[None, :, :]
    spike_list = jnp.sum(jnp.where(spike_matches, spike_length[None, :, :], 0.0), axis=-1)
    return (-per_head_decay[None, :] * decay_factor_lookup[:, None] + spike_list).astype(jnp.float32)


def steps_of(rng, dims, shards, smallest, high):
    def one(axis_at, shards_of):
        draws = jax.random.uniform(jax.random.fold_in(jax.random.fold_in(rng, 6), axis_at), (shards_of,), jnp.float32, smallest / len(shards), high / len(shards))
        return jnp.repeat(jnp.exp(draws), dims[axis_at] // shards_of).reshape((-1,) + (1,) * (len(dims) - axis_at - 1))

    gain = one(*shards[0])
    for cut in shards[1:]:
        gain = gain * one(*cut)
    return gain


def noise(rng, dims, width, most, cuts=(), kind=jnp.bfloat16):
    drawn = width * jax.random.normal(rng, dims, jnp.float32)
    if cuts:
        drawn = drawn * steps_of(rng, dims, cuts, -0.22, 0.18)
    return jnp.clip(drawn, -most, most).astype(kind)


def setup_inputs(seed: int = 0) -> dict:
    splits = jax.random.split(jax.random.key(seed), 15)
    mix_query = noise(splits[0], (SEQUENCE_LENGTH, RETENTION_HEADS * HEAD_DIM), 1.0, 6.0, ((0, 8), (1, 4)))
    mix_key = noise(splits[1], (SEQUENCE_LENGTH, RETENTION_HEADS * HEAD_DIM), 1.0, 6.0, ((0, 8), (1, 4)))
    mix_value = noise(splits[2], (SEQUENCE_LENGTH, RETENTION_HEADS * HEAD_DIM), 1.0, 6.0, ((0, 8), (1, 4)))
    mix_gate = noise(splits[3], (SEQUENCE_LENGTH, RETENTION_HEADS * HEAD_DIM), 1.0, 6.0, ((0, 8), (1, 4)))
    log_decay = draw_log_decay(jax.random.fold_in(splits[14], 71), 0)
    ret_gain = jnp.clip(1.0 + 0.18 * jax.random.normal(splits[5], (RETENTION_HEADS * HEAD_DIM,), jnp.float32), 0.1, 1.9)
    w_out = noise(splits[6], (RETENTION_HEADS * HEAD_DIM, D), (RETENTION_HEADS * HEAD_DIM) ** -0.5, 0.125)
    moe_in = noise(splits[7], (MOE_TOK, D), 1.0, 6.0, ((0, 32),))
    route_ids = draw_route_ids(jax.random.fold_in(splits[14], 71), 0)
    route_weights = jnp.clip(0.1 + 0.9 * jax.random.uniform(splits[9], (MOE_TOK, TOP), jnp.float32) ** steps_of(splits[9], (MOE_TOK, TOP), ((0, 32),), -0.2, 0.2), 0.1, 1.0)
    moe_gain = jnp.clip(1.0 + 0.18 * jax.random.normal(splits[10], (D,), jnp.float32), 0.1, 1.9)
    w_gate = noise(splits[11], (EXPERTS, D, FF), D ** -0.5, 0.125, ((0, 8), (2, 4)))
    w_up = noise(splits[12], (EXPERTS, D, FF), D ** -0.5, 0.125, ((0, 8), (2, 4)))
    w_down = noise(splits[13], (EXPERTS, FF, D), FF ** -0.5, 0.0625, ((0, 8), (1, 4)))
    return dict(mix_query=mix_query, mix_key=mix_key, mix_value=mix_value, mix_gate=mix_gate, log_decay=log_decay, ret_gain=ret_gain, w_out=w_out, moe_in=moe_in, route_ids=route_ids, route_weights=route_weights, moe_gain=moe_gain, w_gate=w_gate, w_up=w_up, w_down=w_down)


norm_eps = 1e-06

def rotate(tensor, position_index):
    head_dim = tensor.shape[-1]
    half_dim = head_dim // 2
    inverse = 10000.0 ** (-(jnp.arange(half_dim, dtype=jnp.float32) * 2.0) / head_dim)
    angle = position_index.astype(jnp.float32)[:, None] * inverse[None, :]
    cosine = jnp.cos(angle)[:, None, :]
    sine = jnp.sin(angle)[:, None, :]
    front = tensor[..., :half_dim]
    back = tensor[..., half_dim:]
    return jnp.concatenate([front * cosine - back * sine, back * cosine + front * sine], axis=-1)

def retention_blocks(query_rot, key_rot, values, log_decay):
    length = query_rot.shape[0]
    block_count = length // BLOCK
    query_blocks = query_rot.reshape(block_count, BLOCK, RETENTION_HEADS, HEAD_DIM)
    key_blocks = key_rot.reshape(block_count, BLOCK, RETENTION_HEADS, HEAD_DIM)
    value_blocks = values.reshape(block_count, BLOCK, RETENTION_HEADS, HEAD_DIM)
    cumulative = jnp.cumsum(log_decay.reshape(block_count, BLOCK, RETENTION_HEADS), axis=1)
    causal = jnp.arange(BLOCK)[:, None] >= jnp.arange(BLOCK)[None, :]

    def advance(carried, block_items):
        query_now, key_now, value_now, cumul_now = block_items
        scores = jnp.einsum('ihd,jhd->hij', query_now.astype(jnp.float32), key_now.astype(jnp.float32))
        by_head = cumul_now.T
        log_gap = by_head[:, :, None] - by_head[:, None, :]
        decay_mask = jnp.where(causal[None], jnp.exp(jnp.where(causal[None], log_gap, 0.0)), 0.0)
        weights = (scores * decay_mask).astype(jnp.bfloat16)
        within_block = jnp.einsum('hij,jhe->ihe', weights.astype(jnp.float32), value_now.astype(jnp.float32))
        block_last = cumul_now[-1]
        query_decayed = query_now.astype(jnp.float32) * jnp.exp(cumul_now)[:, :, None]
        carried_part = jnp.einsum('ihd,hde->ihe', query_decayed, carried, precision=lax.Precision.HIGHEST)
        key_decayed = (key_now.astype(jnp.float32) * jnp.exp(block_last[None, :] - cumul_now)[:, :, None]).astype(jnp.bfloat16)
        update = jnp.einsum('jhd,jhe->hde', key_decayed.astype(jnp.float32), value_now.astype(jnp.float32))
        return (jnp.exp(block_last)[:, None, None] * carried + update, within_block + carried_part)
    initial = jnp.zeros((RETENTION_HEADS, HEAD_DIM, HEAD_DIM), jnp.float32)
    final_state, outputs = lax.scan(advance, initial, (query_blocks, key_blocks, value_blocks, cumulative))
    return outputs.reshape(length, RETENTION_HEADS, HEAD_DIM)

def mixer_reference(mix_query, mix_key, mix_value, mix_gate, log_decay, ret_gain, w_out):
    length = mix_query.shape[0]
    position_index = jnp.arange(length, dtype=jnp.int32)
    query_rot = rotate(mix_query.astype(jnp.float32).reshape(length, RETENTION_HEADS, HEAD_DIM), position_index).astype(jnp.bfloat16)
    key_rot = (rotate(mix_key.astype(jnp.float32).reshape(length, RETENTION_HEADS, HEAD_DIM), position_index) * HEAD_DIM ** (-0.5)).astype(jnp.bfloat16)
    values = mix_value.reshape(length, RETENTION_HEADS, HEAD_DIM)
    retained = retention_blocks(query_rot, key_rot, values, log_decay)
    inverse_rms = lax.rsqrt(lax.optimization_barrier(jnp.mean(retained * retained, axis=-1, keepdims=True)) + norm_eps)
    gate_act = jax.nn.silu(mix_gate.astype(jnp.float32).reshape(length, RETENTION_HEADS, HEAD_DIM))
    heads_out = (gate_act * retained * inverse_rms * ret_gain.reshape(RETENTION_HEADS, HEAD_DIM)).astype(jnp.bfloat16)
    projected = jnp.dot(heads_out.reshape(length, RETENTION_HEADS * HEAD_DIM), w_out, preferred_element_type=jnp.float32)
    return projected.astype(jnp.bfloat16)

def expert_reference(moe_in, route_ids, route_weights, moe_gain, w_gate, w_up, w_down):
    tokens = moe_in.shape[0]
    model_width = moe_in.shape[1]
    block_count = tokens // MOE_DEV
    floats = moe_in.astype(jnp.float32)
    normed = (floats * lax.rsqrt(lax.optimization_barrier(jnp.mean(floats * floats, axis=-1, keepdims=True)) + norm_eps) * moe_gain).astype(jnp.bfloat16)
    block_ids = route_ids.reshape(block_count, MOE_DEV * TOP)
    onehot = (block_ids[:, :, None] == jnp.arange(EXPERTS, dtype=jnp.int32)[None, None, :]).astype(jnp.int32)
    slot_index = lax.optimization_barrier(jnp.sum(jnp.cumsum(onehot, axis=1) * onehot, axis=-1)) - 1
    buffer_rows = (jnp.arange(block_count, dtype=jnp.int32)[:, None] * CAP + slot_index).reshape(-1)
    token_index = (jnp.arange(block_count, dtype=jnp.int32)[:, None] * MOE_DEV + jnp.arange(MOE_DEV * TOP, dtype=jnp.int32)[None, :] // TOP).reshape(-1)
    flat_ids = block_ids.reshape(-1)
    buffer = jnp.zeros((EXPERTS, block_count * CAP, model_width), jnp.bfloat16)
    buffer = buffer.at[flat_ids, buffer_rows].set(normed[token_index])
    group_width = FF // N_TP

    def one_expert(expert_items):
        row_block, gate_weight, up_weight, down_weight = expert_items
        gate_part = jnp.dot(row_block, gate_weight, preferred_element_type=jnp.float32)
        up_part = jnp.dot(row_block, up_weight, preferred_element_type=jnp.float32)
        hidden = (jax.nn.silu(gate_part) * up_part).astype(jnp.bfloat16)
        summed = jnp.zeros((row_block.shape[0], model_width), jnp.float32)
        for group in range(N_TP):
            partial_value = jnp.dot(hidden[:, group * group_width:(group + 1) * group_width], down_weight[group * group_width:(group + 1) * group_width], preferred_element_type=jnp.float32).astype(jnp.bfloat16)
            summed = summed + partial_value.astype(jnp.float32)
        return summed.astype(jnp.bfloat16)
    outputs = lax.map(one_expert, (buffer, w_gate, w_up, w_down))
    picked = outputs[flat_ids, buffer_rows].reshape(tokens, TOP, model_width)
    combined = lax.optimization_barrier(jnp.sum(picked.astype(jnp.float32) * route_weights[:, :, None], axis=1))
    return combined.astype(jnp.bfloat16)

def reference(mix_query, mix_key, mix_value, mix_gate, log_decay, ret_gain, w_out, moe_in, route_ids, route_weights, moe_gain, w_gate, w_up, w_down):
    mix_out = mixer_reference(mix_query, mix_key, mix_value, mix_gate, log_decay, ret_gain, w_out)
    moe_out = expert_reference(moe_in, route_ids, route_weights, moe_gain, w_gate, w_up, w_down)
    return (mix_out, moe_out)
```

```python
import functools

import jax
import jax.numpy as jnp
import numpy as np
from jax import lax
from jax.experimental import pallas as pl
from jax.experimental.pallas import tpu as pltpu
from jax.sharding import PartitionSpec as P

HEAD_DIM = 256
BLOCK = 512
norm_eps = 1e-06
F32 = jnp.float32
BF16 = jnp.bfloat16
VMEM_LIMIT = 60 * 1024 * 1024
TAIL = 16


def params(*semantics):
    return pltpu.CompilerParams(
        dimension_semantics=semantics or None, vmem_limit_bytes=VMEM_LIMIT
    )


def cost(flops, moved, exps=0):
    return pl.CostEstimate(flops=int(flops), bytes_accessed=int(moved), transcendentals=int(exps))


def dot(a, b, ca=1, cb=0):
    return lax.dot_general(a, b, (((ca,), (cb,)), ((), ())), preferred_element_type=F32)


def split3(x):
    a = x.astype(BF16)
    rest = x - a.astype(F32)
    b = rest.astype(BF16)
    c = (rest - b.astype(F32)).astype(BF16)
    return a, b, c


def retention_kernel(
    slices, place_ref, q_ref, k_ref, v_ref, l_ref, cos_r, sin_r, cos_b, sin_b,
    local_ref, qd_ref, message_ref, state, before,
):
    head = pl.program_id(0)
    block = pl.program_id(1)
    size = q_ref.shape[0]
    half = HEAD_DIM // 2

    @pl.when(block == 0)
    def _():
        state[...] = jnp.zeros_like(state)
        before[...] = jnp.zeros_like(before)

    rows = lax.broadcasted_iota(jnp.int32, (size, size), 0)
    cols = lax.broadcasted_iota(jnp.int32, (size, size), 1)
    upper = jnp.where(rows <= cols, 1.0, 0.0).astype(BF16)
    a, b, c = split3(l_ref[...])
    sums = dot(a, upper) + dot(b, upper) + dot(c, upper)
    pick = lax.broadcasted_iota(jnp.int32, sums.shape, 0) == head
    cum_row = jnp.sum(jnp.where(pick, sums, 0.0), axis=0, keepdims=True)
    cum_col = jnp.transpose(jnp.broadcast_to(cum_row, (8, size)))[:, 0:1]
    last = cum_row[:, size - 1 : size]

    cb, sb = cos_b[0], sin_b[0]
    cosine = cos_r[...] * cb - sin_r[...] * sb
    sine = sin_r[...] * cb + cos_r[...] * sb

    def rotate(x):
        front = x[:, :half].astype(F32)
        back = x[:, half:].astype(F32)
        return jnp.concatenate(
            [front * cosine - back * sine, back * cosine + front * sine], axis=1
        )

    q_rot = rotate(q_ref[...]).astype(BF16)
    k_rot = (rotate(k_ref[...]) * HEAD_DIM ** (-0.5)).astype(BF16)
    value = v_ref[...]
    q_wide = q_rot.astype(F32)
    grown = before[0:1, 0:1]
    decay_in = jnp.exp(cum_col)
    q_decayed = (q_wide * decay_in).astype(BF16)
    qd_ref[...] = (q_wide * jnp.exp(cum_col + grown)).astype(BF16)
    old = state[...]
    carried = dot(q_decayed, old.astype(BF16))
    step = size // 2
    for i in range(2):
        r0, width = i * step, (i + 1) * step
        scores = dot(q_rot[r0 : r0 + step], k_rot[:width], 1, 1)
        causal = (
            lax.broadcasted_iota(jnp.int32, (step, width), 0) + r0
            >= lax.broadcasted_iota(jnp.int32, (step, width), 1)
        )
        gap = cum_col[r0 : r0 + step] - cum_row[:, :width]
        mask = jnp.exp(jnp.where(causal, gap, -1e30))
        weights = (scores * mask).astype(BF16)
        local_ref[r0 : r0 + step, :] = dot(weights, value[:width]) + carried[r0 : r0 + step]
    k_decayed = (k_rot.astype(F32) * jnp.exp(last - cum_col)).astype(BF16)
    fresh = jnp.exp(last) * old + dot(k_decayed, value, 0, 0)
    state[...] = fresh
    before[...] = before[...] + last

    @pl.when(block == pl.num_programs(1) - 1)
    def _():
        part = HEAD_DIM // slices
        total = jnp.exp(before[0:1, 0:1])
        tail = jnp.broadcast_to(total, (TAIL, HEAD_DIM)).astype(BF16)
        for i in range(slices):
            message_ref[i, :part, :] = fresh[i * part : (i + 1) * part].astype(BF16)
            message_ref[i, part:, :] = tail


def retention(mix_query, mix_key, mix_value, log_decay, devices, place):
    rows, width = mix_query.shape
    heads = width // HEAD_DIM
    blocks = rows // BLOCK
    half = HEAD_DIM // 2
    slices = devices // heads
    part = HEAD_DIM // slices
    inverse = 10000.0 ** (-(np.arange(half) * 2.0) / HEAD_DIM)
    fine = np.arange(BLOCK)[:, None] * inverse[None, :]
    coarse = (np.arange(devices * blocks) * BLOCK)[:, None, None] * inverse[None, None, :]
    tables = [np.asarray(f(x), np.float32) for x in (fine, coarse) for f in (np.cos, np.sin)]
    logs = jnp.pad(log_decay.T, ((0, 8 - heads), (0, 0)))
    tile = pl.BlockSpec((BLOCK, HEAD_DIM), lambda h, b, p: (b, h))
    whole = pl.BlockSpec((BLOCK, half), lambda h, b, p: (0, 0))
    base = pl.BlockSpec((1, 1, half), lambda h, b, p: (p[0] * blocks + b, 0, 0))
    return pl.pallas_call(
        functools.partial(retention_kernel, slices),
        grid_spec=pltpu.PrefetchScalarGridSpec(
            num_scalar_prefetch=1,
            grid=(heads, blocks),
            in_specs=[
                tile, tile, tile,
                pl.BlockSpec((8, BLOCK), lambda h, b, p: (0, b)),
                whole, whole, base, base,
            ],
            out_specs=[
                tile, tile,
                pl.BlockSpec((slices, part + TAIL, HEAD_DIM), lambda h, b, p: (h, 0, 0)),
            ],
            scratch_shapes=[pltpu.VMEM((HEAD_DIM, HEAD_DIM), F32), pltpu.VMEM((8, 128), F32)],
        ),
        out_shape=[
            jax.ShapeDtypeStruct((rows, width), F32),
            jax.ShapeDtypeStruct((rows, width), BF16),
            jax.ShapeDtypeStruct((devices, part + TAIL, HEAD_DIM), BF16),
        ],
        compiler_params=params("arbitrary", "arbitrary"),
        cost_estimate=cost(rows * width * (4 * BLOCK + 4 * HEAD_DIM) * 2, rows * width * 12),
        name="retention",
    )(place, mix_query, mix_key, mix_value, logs, tables[0], tables[1], tables[2], tables[3])


def prefix_kernel(in_ref, out_ref):
    part = out_ref.shape[1]
    state = jnp.zeros(out_ref.shape[1:], F32)
    for s in range(out_ref.shape[0]):
        out_ref[s] = state.astype(BF16)
        state = in_ref[s, part : part + 1, :].astype(F32) * state + in_ref[s, :part, :].astype(F32)


def prefix(messages):
    devices, length, width = messages.shape
    return pl.pallas_call(
        prefix_kernel,
        out_shape=jax.ShapeDtypeStruct((devices, length - TAIL, width), BF16),
        compiler_params=params(),
        cost_estimate=cost(messages.size * 2, messages.size * 4),
        name="prefix",
    )(messages)


def finish_kernel(local_ref, qd_ref, in_ref, gate_ref, gain_ref, out_ref):
    retained = local_ref[...] + dot(qd_ref[...], in_ref[0])
    inverse_rms = lax.rsqrt(jnp.mean(retained * retained, axis=-1, keepdims=True) + norm_eps)
    gate = gate_ref[...].astype(F32)
    gate = gate / (1.0 + jnp.exp(-gate))
    out_ref[...] = (gate * retained * inverse_rms * gain_ref[...]).astype(BF16)


def finish(head, local, q_decayed, incoming, mix_gate, ret_gain):
    rows = local.shape[0]
    tile = pl.BlockSpec((BLOCK, HEAD_DIM), lambda b: (b, head))
    return pl.pallas_call(
        finish_kernel,
        grid=(rows // BLOCK,),
        in_specs=[
            tile, tile,
            pl.BlockSpec((1, HEAD_DIM, HEAD_DIM), lambda b: (head, 0, 0)),
            tile,
            pl.BlockSpec((1, HEAD_DIM), lambda b: (0, head)),
        ],
        out_specs=pl.BlockSpec((BLOCK, HEAD_DIM), lambda b: (b, 0)),
        out_shape=jax.ShapeDtypeStruct((rows, HEAD_DIM), BF16),
        compiler_params=params("arbitrary"),
        cost_estimate=cost(rows * HEAD_DIM * HEAD_DIM * 2, rows * HEAD_DIM * 10),
        name="finish",
    )(local, q_decayed, incoming, mix_gate, ret_gain)


def project_kernel(lanes, heads, *refs):
    pieces, w_ref, out_ref = refs[:heads], refs[heads], refs[heads + 1]
    total = None
    for h in range(heads):
        for lane in range(lanes):
            r0 = (lane * heads + h) * HEAD_DIM
            term = dot(pieces[h][lane], w_ref[r0 : r0 + HEAD_DIM, :])
            total = term if total is None else total + term
    out_ref[...] = total.astype(BF16)


def project(pieces, w_out):
    heads = len(pieces)
    lanes, rows, _ = pieces[0].shape
    depth, width = w_out.shape
    tile = 256
    return pl.pallas_call(
        functools.partial(project_kernel, lanes, heads),
        grid=(width // tile,),
        in_specs=[pl.BlockSpec((lanes, rows, HEAD_DIM), lambda n: (0, 0, 0))] * heads
        + [pl.BlockSpec((depth, tile), lambda n: (0, n))],
        out_specs=pl.BlockSpec((rows, tile), lambda n: (0, n)),
        out_shape=jax.ShapeDtypeStruct((rows, width), BF16),
        compiler_params=params("arbitrary"),
        cost_estimate=cost(2 * rows * depth * width, 2 * (rows * depth + depth * width)),
        name="project",
    )(*pieces, w_out)


def slots_of(ids, capacity, count):
    tokens = ids.shape[0]
    lane = lax.broadcasted_iota(jnp.int32, (tokens, count), 1)
    expert = lane // capacity
    first = ids[:, 0:1] == expert
    second = ids[:, 1:2] == expert
    member = jnp.where(first | second, 1.0, 0.0)
    earlier = jnp.where(
        lax.broadcasted_iota(jnp.int32, (tokens, tokens), 0)
        > lax.broadcasted_iota(jnp.int32, (tokens, tokens), 1),
        1.0,
        0.0,
    ).astype(BF16)
    taken = dot(earlier, member.astype(BF16))
    slot = (lane - expert * capacity).astype(F32)
    return jnp.where(taken == slot, member, 0.0), first


def dispatch_kernel(capacity, x_ref, ids_ref, gain_ref, out_ref):
    floats = x_ref[...].astype(F32)
    scale = lax.rsqrt(jnp.mean(floats * floats, axis=-1, keepdims=True) + norm_eps)
    normed = (floats * scale * gain_ref[...]).astype(BF16)
    chosen, _ = slots_of(ids_ref[...], capacity, out_ref.shape[0])
    out_ref[...] = dot(chosen.astype(BF16), normed, 0, 0).astype(BF16)


def dispatch(moe_in, route_ids, moe_gain, experts, capacity):
    width = moe_in.shape[1]
    return pl.pallas_call(
        functools.partial(dispatch_kernel, capacity),
        out_shape=jax.ShapeDtypeStruct((experts * capacity, width), BF16),
        compiler_params=params(),
        cost_estimate=cost(moe_in.size * 256, moe_in.size * 8),
        name="dispatch",
    )(moe_in, route_ids, moe_gain.reshape(1, width))


def combine_kernel(capacity, x_ref, ids_ref, w_ref, out_ref):
    chosen, first = slots_of(ids_ref[...], capacity, x_ref.shape[0])
    weight = chosen * jnp.where(first, w_ref[:, 0:1], w_ref[:, 1:2])
    x = x_ref[...]
    total = None
    for term in split3(weight):
        part = dot(term, x)
        total = part if total is None else total + part
    out_ref[...] = total.astype(BF16)


def combine(returned, route_ids, route_weights, capacity):
    tokens = route_ids.shape[0]
    return pl.pallas_call(
        functools.partial(combine_kernel, capacity),
        out_shape=jax.ShapeDtypeStruct((tokens, returned.shape[1]), BF16),
        compiler_params=params(),
        cost_estimate=cost(returned.size * 200, returned.size * 4),
        name="combine",
    )(returned, route_ids, route_weights)


def up_kernel(count, *refs):
    pieces, g_ref, u_ref, out_ref, x = refs[:count], *refs[count:]
    rows = pieces[0].shape[0]

    @pl.when(pl.program_id(0) == 0)
    def _():
        for i in range(count):
            x[i * rows : (i + 1) * rows, :] = pieces[i][...]

    gate = dot(x[...], g_ref[0])
    up = dot(x[...], u_ref[0])
    out_ref[...] = (gate / (1.0 + jnp.exp(-gate)) * up).astype(BF16)


def expert_up(pieces, w_gate, w_up):
    count = len(pieces)
    rows, depth = pieces[0].shape
    width = w_gate.shape[2]
    tile = 256 if width % 256 == 0 else 128
    weight = pl.BlockSpec((1, depth, tile), lambda n: (0, 0, n))
    total = rows * count
    return pl.pallas_call(
        functools.partial(up_kernel, count),
        grid=(width // tile,),
        in_specs=[pl.BlockSpec((rows, depth), lambda n: (0, 0))] * count + [weight, weight],
        out_specs=pl.BlockSpec((total, tile), lambda n: (0, n)),
        out_shape=jax.ShapeDtypeStruct((total, width), BF16),
        scratch_shapes=[pltpu.VMEM((total, depth), BF16)],
        compiler_params=params("arbitrary"),
        cost_estimate=cost(4 * total * depth * width, 4 * depth * width),
        name="expert_up",
    )(*pieces, w_gate, w_up)


def down_kernel(h_ref, w_ref, keep_ref, send_ref):
    y = dot(h_ref[...], w_ref[0]).astype(BF16)
    rows = keep_ref.shape[0]
    keep_ref[...] = y[:rows]
    send_ref[...] = y[rows:]


def expert_down(hidden, w_down):
    rows, depth = hidden.shape
    width = w_down.shape[2]
    tile = 256
    out = pl.BlockSpec((rows // 2, tile), lambda n: (0, n))
    return pl.pallas_call(
        down_kernel,
        grid=(width // tile,),
        in_specs=[
            pl.BlockSpec((rows, depth), lambda n: (0, 0)),
            pl.BlockSpec((1, depth, tile), lambda n: (0, 0, n)),
        ],
        out_specs=[out, out],
        out_shape=[jax.ShapeDtypeStruct((rows // 2, width), BF16)] * 2,
        compiler_params=params("arbitrary"),
        cost_estimate=cost(2 * rows * depth * width, 2 * depth * width),
        name="expert_down",
    )(hidden, w_down)


def exchange(x, axis):
    return lax.all_to_all(x, axis, split_axis=0, concat_axis=0, tiled=True)


def to_core(x, lanes):
    return lax.ppermute(x, "tp", [(i, i ^ 1) for i in range(lanes)])


def to_chip(x, shift, lanes):
    return lax.ppermute(x, "tp", [(i, (i + 2 * shift) % lanes) for i in range(lanes)])


def on_device(
    mix_query, mix_key, mix_value, mix_gate, log_decay, ret_gain, w_out,
    moe_in, route_ids, route_weights, moe_gain, w_gate, w_up, w_down,
):
    devices = lax.axis_size("ep")
    lanes = lax.axis_size("tp")
    chips = lanes // 2
    place = lax.axis_index("ep").astype(jnp.int32).reshape(1)
    heads = mix_query.shape[1] // HEAD_DIM
    tokens, model_width = moe_in.shape
    capacity = 4 * tokens // devices

    outgoing = dispatch(moe_in, route_ids, moe_gain, devices, capacity)
    own = exchange(outgoing, "ep")

    local, q_decayed, message = retention(
        mix_query, mix_key, mix_value, log_decay, devices, place
    )
    incoming = exchange(prefix(exchange(message, "ep")), "ep")
    incoming = incoming.reshape(heads, HEAD_DIM, HEAD_DIM)

    near = [own] + [to_chip(own, s, lanes) for s in range(1, chips)]
    pieces = near + [to_core(x, lanes) for x in near]

    gain = ret_gain.reshape(1, -1)
    gathered = []
    for h in range(heads):
        out = finish(h, local, q_decayed, incoming, mix_gate, gain)
        gathered.append(exchange(out.reshape(lanes, -1, HEAD_DIM), "tp"))

    hidden = expert_up(pieces, w_gate, w_up)
    keep, send = expert_down(hidden, w_down)
    joined = (keep.astype(F32) + to_core(send, lanes).astype(F32)).astype(BF16)
    joined = joined.reshape(chips, -1, model_width)
    total = joined[0].astype(F32)
    for s in range(1, chips):
        total = total + to_chip(joined[s], -s, lanes).astype(F32)
    returned = exchange(total.astype(BF16), "ep")
    moe_out = combine(returned, route_ids, route_weights, capacity)
    mix_out = project(gathered, w_out)
    return (mix_out, moe_out)


def solution(mesh):
    in_specs = (
        P("ep", "tp"),
        P("ep", "tp"),
        P("ep", "tp"),
        P("ep", "tp"),
        P("ep", "tp"),
        P("tp"),
        P(),
        P(("ep", "tp"), None),
        P(("ep", "tp"), None),
        P(("ep", "tp"), None),
        P(),
        P("ep", None, "tp"),
        P("ep", None, "tp"),
        P("ep", "tp", None),
    )
    out_specs = (P(("ep", "tp"), None), P(("ep", "tp"), None))
    return jax.shard_map(
        on_device, mesh=mesh, in_specs=in_specs, out_specs=out_specs, check_vma=False
    )
```

```python
import functools

import jax
import jax.numpy as jnp
import numpy as np
from jax import lax
from jax.experimental import pallas as pl
from jax.experimental.pallas import tpu as pltpu
from jax.sharding import PartitionSpec as P

HEAD_DIM = 256
BLOCK = 512
norm_eps = 1e-06
F32 = jnp.float32
BF16 = jnp.bfloat16
VMEM_LIMIT = 60 * 1024 * 1024
TAIL = 16


def params(*semantics):
    return pltpu.CompilerParams(
        dimension_semantics=semantics or None, vmem_limit_bytes=VMEM_LIMIT
    )


def cost(flops, moved, exps=0):
    return pl.CostEstimate(flops=int(flops), bytes_accessed=int(moved), transcendentals=int(exps))


def dot(a, b, ca=1, cb=0):
    return lax.dot_general(a, b, (((ca,), (cb,)), ((), ())), preferred_element_type=F32)


def split3(x):
    a = x.astype(BF16)
    rest = x - a.astype(F32)
    b = rest.astype(BF16)
    c = (rest - b.astype(F32)).astype(BF16)
    return a, b, c


def retention_kernel(
    slices, place_ref, q_ref, k_ref, v_ref, l_ref, cos_r, sin_r, cos_b, sin_b,
    local_ref, qd_ref, message_ref, state, before,
):
    head = pl.program_id(0)
    block = pl.program_id(1)
    size = q_ref.shape[0]
    half = HEAD_DIM // 2

    @pl.when(block == 0)
    def _():
        state[...] = jnp.zeros_like(state)
        before[...] = jnp.zeros_like(before)

    rows = lax.broadcasted_iota(jnp.int32, (size, size), 0)
    cols = lax.broadcasted_iota(jnp.int32, (size, size), 1)
    upper = jnp.where(rows <= cols, 1.0, 0.0).astype(BF16)
    a, b, c = split3(l_ref[...])
    sums = dot(a, upper) + dot(b, upper) + dot(c, upper)
    pick = lax.broadcasted_iota(jnp.int32, sums.shape, 0) == head
    cum_row = jnp.sum(jnp.where(pick, sums, 0.0), axis=0, keepdims=True)
    cum_col = jnp.transpose(jnp.broadcast_to(cum_row, (8, size)))[:, 0:1]
    last = cum_row[:, size - 1 : size]

    cb, sb = cos_b[0], sin_b[0]
    cosine = cos_r[...] * cb - sin_r[...] * sb
    sine = sin_r[...] * cb + cos_r[...] * sb

    def rotate(x):
        front = x[:, :half].astype(F32)
        back = x[:, half:].astype(F32)
        return jnp.concatenate(
            [front * cosine - back * sine, back * cosine + front * sine], axis=1
        )

    q_rot = rotate(q_ref[...]).astype(BF16)
    k_rot = (rotate(k_ref[...]) * HEAD_DIM ** (-0.5)).astype(BF16)
    value = v_ref[...]
    q_wide = q_rot.astype(F32)
    grown = before[0:1, 0:1]
    decay_in = jnp.exp(cum_col)
    q_decayed = (q_wide * decay_in).astype(BF16)
    qd_ref[...] = (q_wide * jnp.exp(cum_col + grown)).astype(BF16)
    old = state[...]
    carried = dot(q_decayed, old.astype(BF16))
    step = size // 2
    for i in range(2):
        r0, width = i * step, (i + 1) * step
        scores = dot(q_rot[r0 : r0 + step], k_rot[:width], 1, 1)
        causal = (
            lax.broadcasted_iota(jnp.int32, (step, width), 0) + r0
            >= lax.broadcasted_iota(jnp.int32, (step, width), 1)
        )
        gap = cum_col[r0 : r0 + step] - cum_row[:, :width]
        mask = jnp.exp(jnp.where(causal, gap, -1e30))
        weights = (scores * mask).astype(BF16)
        local_ref[r0 : r0 + step, :] = dot(weights, value[:width]) + carried[r0 : r0 + step]
    k_decayed = (k_rot.astype(F32) * jnp.exp(last - cum_col)).astype(BF16)
    fresh = jnp.exp(last) * old + dot(k_decayed, value, 0, 0)
    state[...] = fresh
    before[...] = before[...] + last

    @pl.when(block == pl.num_programs(1) - 1)
    def _():
        part = HEAD_DIM // slices
        total = jnp.exp(before[0:1, 0:1])
        tail = jnp.broadcast_to(total, (TAIL, HEAD_DIM)).astype(BF16)
        for i in range(slices):
            message_ref[i, :part, :] = fresh[i * part : (i + 1) * part].astype(BF16)
            message_ref[i, part:, :] = tail


def retention(mix_query, mix_key, mix_value, log_decay, devices, place):
    rows, width = mix_query.shape
    heads = width // HEAD_DIM
    blocks = rows // BLOCK
    half = HEAD_DIM // 2
    slices = devices // heads
    part = HEAD_DIM // slices
    inverse = 10000.0 ** (-(np.arange(half) * 2.0) / HEAD_DIM)
    fine = np.arange(BLOCK)[:, None] * inverse[None, :]
    coarse = (np.arange(devices * blocks) * BLOCK)[:, None, None] * inverse[None, None, :]
    tables = [np.asarray(f(x), np.float32) for x in (fine, coarse) for f in (np.cos, np.sin)]
    logs = jnp.pad(log_decay.T, ((0, 8 - heads), (0, 0)))
    tile = pl.BlockSpec((BLOCK, HEAD_DIM), lambda h, b, p: (b, h))
    whole = pl.BlockSpec((BLOCK, half), lambda h, b, p: (0, 0))
    base = pl.BlockSpec((1, 1, half), lambda h, b, p: (p[0] * blocks + b, 0, 0))
    return pl.pallas_call(
        functools.partial(retention_kernel, slices),
        grid_spec=pltpu.PrefetchScalarGridSpec(
            num_scalar_prefetch=1,
            grid=(heads, blocks),
            in_specs=[
                tile, tile, tile,
                pl.BlockSpec((8, BLOCK), lambda h, b, p: (0, b)),
                whole, whole, base, base,
            ],
            out_specs=[
                tile, tile,
                pl.BlockSpec((slices, part + TAIL, HEAD_DIM), lambda h, b, p: (h, 0, 0)),
            ],
            scratch_shapes=[pltpu.VMEM((HEAD_DIM, HEAD_DIM), F32), pltpu.VMEM((8, 128), F32)],
        ),
        out_shape=[
            jax.ShapeDtypeStruct((rows, width), F32),
            jax.ShapeDtypeStruct((rows, width), BF16),
            jax.ShapeDtypeStruct((devices, part + TAIL, HEAD_DIM), BF16),
        ],
        compiler_params=params("arbitrary", "arbitrary"),
        cost_estimate=cost(rows * width * (4 * BLOCK + 4 * HEAD_DIM) * 2, rows * width * 12),
        name="retention",
    )(place, mix_query, mix_key, mix_value, logs, tables[0], tables[1], tables[2], tables[3])


def prefix_kernel(in_ref, out_ref):
    part = out_ref.shape[1]
    state = jnp.zeros(out_ref.shape[1:], F32)
    for s in range(out_ref.shape[0]):
        out_ref[s] = state.astype(BF16)
        state = in_ref[s, part : part + 1, :].astype(F32) * state + in_ref[s, :part, :].astype(F32)


def prefix(messages):
    devices, length, width = messages.shape
    return pl.pallas_call(
        prefix_kernel,
        out_shape=jax.ShapeDtypeStruct((devices, length - TAIL, width), BF16),
        compiler_params=params(),
        cost_estimate=cost(messages.size * 2, messages.size * 4),
        name="prefix",
    )(messages)


def finish_kernel(local_ref, qd_ref, in_ref, gate_ref, gain_ref, out_ref):
    retained = local_ref[...] + dot(qd_ref[...], in_ref[0])
    inverse_rms = lax.rsqrt(jnp.mean(retained * retained, axis=-1, keepdims=True) + norm_eps)
    gate = gate_ref[...].astype(F32)
    gate = gate / (1.0 + jnp.exp(-gate))
    out_ref[...] = (gate * retained * inverse_rms * gain_ref[...]).astype(BF16)


def finish(local, q_decayed, incoming, mix_gate, ret_gain):
    rows, width = local.shape
    tile = pl.BlockSpec((BLOCK, HEAD_DIM), lambda h, b: (b, h))
    return pl.pallas_call(
        finish_kernel,
        grid=(width // HEAD_DIM, rows // BLOCK),
        in_specs=[
            tile, tile,
            pl.BlockSpec((1, HEAD_DIM, HEAD_DIM), lambda h, b: (h, 0, 0)),
            tile,
            pl.BlockSpec((1, HEAD_DIM), lambda h, b: (0, h)),
        ],
        out_specs=tile,
        out_shape=jax.ShapeDtypeStruct((rows, width), BF16),
        compiler_params=params("arbitrary", "arbitrary"),
        cost_estimate=cost(rows * width * HEAD_DIM * 2, rows * width * 10),
        name="finish",
    )(local, q_decayed, incoming, mix_gate, ret_gain)


def project_kernel(x_ref, w_ref, out_ref, x):
    lanes, _, width = x_ref.shape

    @pl.when(pl.program_id(0) == 0)
    def _():
        for lane in range(lanes):
            x[:, lane * width : (lane + 1) * width] = x_ref[lane]

    out_ref[...] = dot(x[...], w_ref[...]).astype(BF16)


def project(gathered, w_out):
    lanes, rows, part = gathered.shape
    depth, width = w_out.shape
    tile = 512
    return pl.pallas_call(
        project_kernel,
        grid=(width // tile,),
        in_specs=[
            pl.BlockSpec((lanes, rows, part), lambda n: (0, 0, 0)),
            pl.BlockSpec((depth, tile), lambda n: (0, n)),
        ],
        out_specs=pl.BlockSpec((rows, tile), lambda n: (0, n)),
        out_shape=jax.ShapeDtypeStruct((rows, width), BF16),
        scratch_shapes=[pltpu.VMEM((rows, depth), BF16)],
        compiler_params=params("arbitrary"),
        cost_estimate=cost(2 * rows * depth * width, 2 * (rows * depth + depth * width)),
        name="project",
    )(gathered, w_out)


def slots_of(ids, capacity, count):
    tokens = ids.shape[0]
    lane = lax.broadcasted_iota(jnp.int32, (tokens, count), 1)
    expert = lane // capacity
    first = ids[:, 0:1] == expert
    second = ids[:, 1:2] == expert
    member = jnp.where(first | second, 1.0, 0.0)
    earlier = jnp.where(
        lax.broadcasted_iota(jnp.int32, (tokens, tokens), 0)
        > lax.broadcasted_iota(jnp.int32, (tokens, tokens), 1),
        1.0,
        0.0,
    ).astype(BF16)
    taken = dot(earlier, member.astype(BF16))
    slot = (lane - expert * capacity).astype(F32)
    return jnp.where(taken == slot, member, 0.0), first


def dispatch_kernel(capacity, x_ref, ids_ref, gain_ref, out_ref):
    floats = x_ref[...].astype(F32)
    scale = lax.rsqrt(jnp.mean(floats * floats, axis=-1, keepdims=True) + norm_eps)
    normed = (floats * scale * gain_ref[...]).astype(BF16)
    chosen, _ = slots_of(ids_ref[...], capacity, out_ref.shape[0])
    out_ref[...] = dot(chosen.astype(BF16), normed, 0, 0).astype(BF16)


def dispatch(moe_in, route_ids, moe_gain, experts, capacity):
    width = moe_in.shape[1]
    return pl.pallas_call(
        functools.partial(dispatch_kernel, capacity),
        out_shape=jax.ShapeDtypeStruct((experts * capacity, width), BF16),
        compiler_params=params(),
        cost_estimate=cost(moe_in.size * 256, moe_in.size * 8),
        name="dispatch",
    )(moe_in, route_ids, moe_gain.reshape(1, width))


def combine_kernel(capacity, x_ref, ids_ref, w_ref, out_ref):
    chosen, first = slots_of(ids_ref[...], capacity, x_ref.shape[0])
    weight = chosen * jnp.where(first, w_ref[:, 0:1], w_ref[:, 1:2])
    x = x_ref[...]
    total = None
    for term in split3(weight):
        part = dot(term, x)
        total = part if total is None else total + part
    out_ref[...] = total.astype(BF16)


def combine(returned, route_ids, route_weights, capacity):
    tokens = route_ids.shape[0]
    return pl.pallas_call(
        functools.partial(combine_kernel, capacity),
        out_shape=jax.ShapeDtypeStruct((tokens, returned.shape[1]), BF16),
        compiler_params=params(),
        cost_estimate=cost(returned.size * 200, returned.size * 4),
        name="combine",
    )(returned, route_ids, route_weights)


def up_kernel(count, *refs):
    pieces, g_ref, u_ref, out_ref, x = refs[:count], *refs[count:]
    rows = pieces[0].shape[0]

    @pl.when(pl.program_id(0) == 0)
    def _():
        for i in range(count):
            x[i * rows : (i + 1) * rows, :] = pieces[i][...]

    gate = dot(x[...], g_ref[0])
    up = dot(x[...], u_ref[0])
    out_ref[...] = (gate / (1.0 + jnp.exp(-gate)) * up).astype(BF16)


def expert_up(pieces, w_gate, w_up):
    count = len(pieces)
    rows, depth = pieces[0].shape
    width = w_gate.shape[2]
    tile = 256 if width % 256 == 0 else 128
    weight = pl.BlockSpec((1, depth, tile), lambda n: (0, 0, n))
    total = rows * count
    return pl.pallas_call(
        functools.partial(up_kernel, count),
        grid=(width // tile,),
        in_specs=[pl.BlockSpec((rows, depth), lambda n: (0, 0))] * count + [weight, weight],
        out_specs=pl.BlockSpec((total, tile), lambda n: (0, n)),
        out_shape=jax.ShapeDtypeStruct((total, width), BF16),
        scratch_shapes=[pltpu.VMEM((total, depth), BF16)],
        compiler_params=params("arbitrary"),
        cost_estimate=cost(4 * total * depth * width, 4 * depth * width),
        name="expert_up",
    )(*pieces, w_gate, w_up)


def down_kernel(h_ref, w_ref, keep_ref, send_ref):
    y = dot(h_ref[...], w_ref[0]).astype(BF16)
    rows = keep_ref.shape[0]
    keep_ref[...] = y[:rows]
    send_ref[...] = y[rows:]


def expert_down(hidden, w_down):
    rows, depth = hidden.shape
    width = w_down.shape[2]
    tile = 512
    out = pl.BlockSpec((rows // 2, tile), lambda n: (0, n))
    return pl.pallas_call(
        down_kernel,
        grid=(width // tile,),
        in_specs=[
            pl.BlockSpec((rows, depth), lambda n: (0, 0)),
            pl.BlockSpec((1, depth, tile), lambda n: (0, 0, n)),
        ],
        out_specs=[out, out],
        out_shape=[jax.ShapeDtypeStruct((rows // 2, width), BF16)] * 2,
        compiler_params=params("arbitrary"),
        cost_estimate=cost(2 * rows * depth * width, 2 * depth * width),
        name="expert_down",
    )(hidden, w_down)


def exchange(x, axis):
    return lax.all_to_all(x, axis, split_axis=0, concat_axis=0, tiled=True)


def to_core(x, lanes):
    return lax.ppermute(x, "tp", [(i, i ^ 1) for i in range(lanes)])


def to_chip(x, shift, lanes):
    return lax.ppermute(x, "tp", [(i, (i + 2 * shift) % lanes) for i in range(lanes)])


def on_device(
    mix_query, mix_key, mix_value, mix_gate, log_decay, ret_gain, w_out,
    moe_in, route_ids, route_weights, moe_gain, w_gate, w_up, w_down,
):
    devices = lax.axis_size("ep")
    lanes = lax.axis_size("tp")
    chips = lanes // 2
    place = lax.axis_index("ep").astype(jnp.int32).reshape(1)
    heads = mix_query.shape[1] // HEAD_DIM
    tokens, model_width = moe_in.shape
    capacity = 4 * tokens // devices

    outgoing = dispatch(moe_in, route_ids, moe_gain, devices, capacity)
    own = exchange(outgoing, "ep")

    local, q_decayed, message = retention(
        mix_query, mix_key, mix_value, log_decay, devices, place
    )
    own, message = lax.optimization_barrier((own, message))
    arrived = exchange(message, "ep")
    starts = prefix(arrived)
    incoming = exchange(starts, "ep")
    incoming = incoming.reshape(heads, HEAD_DIM, HEAD_DIM)

    near = [own] + [to_chip(own, s, lanes) for s in range(1, chips)]
    pieces = near + [to_core(x, lanes) for x in near]

    gain = ret_gain.reshape(1, -1)
    mixed = finish(local, q_decayed, incoming, mix_gate, gain)
    *pieces, mixed = lax.optimization_barrier((*pieces, mixed))
    gathered = exchange(mixed.reshape(lanes, -1, mixed.shape[1]), "tp")

    hidden = expert_up(pieces, w_gate, w_up)
    keep, send = expert_down(hidden, w_down)
    joined = (keep.astype(F32) + to_core(send, lanes).astype(F32)).astype(BF16)
    joined = joined.reshape(chips, -1, model_width)
    total = joined[0].astype(F32)
    for s in range(1, chips):
        total = total + to_chip(joined[s], -s, lanes).astype(F32)
    returned = exchange(total.astype(BF16), "ep")
    moe_out = combine(returned, route_ids, route_weights, capacity)
    mix_out = project(gathered, w_out)
    return (mix_out, moe_out)


def solution(mesh):
    in_specs = (
        P("ep", "tp"),
        P("ep", "tp"),
        P("ep", "tp"),
        P("ep", "tp"),
        P("ep", "tp"),
        P("tp"),
        P(),
        P(("ep", "tp"), None),
        P(("ep", "tp"), None),
        P(("ep", "tp"), None),
        P(),
        P("ep", None, "tp"),
        P("ep", None, "tp"),
        P("ep", "tp", None),
    )
    out_specs = (P(("ep", "tp"), None), P(("ep", "tp"), None))

    return jax.shard_map(
        on_device, mesh=mesh, in_specs=in_specs, out_specs=out_specs, check_vma=False
    )
```
